32 devices in a mesh: sp: 16 (over z, y, x), tp: 2 (over core).
Axes of the slice: x: 2, y: 2, z: 4, core: 2. Of those that a mesh axis runs over, the one named last changes fastest.
Arguments:
- tokens: bfloat16 [2048, 2048], P('sp'), may hold values from -6 to 6
- input_norm_scale: float32 [2048], replicated, may hold values from 0.1 to 1.9
- input_norm_bias: float32 [2048], replicated, may hold values from -2 to 2
- query_projection: bfloat16 [2048, 1024], P('sp', 'tp'), may hold values from -0.125 to 0.125
- key_projection: bfloat16 [2048, 1024], P('sp', 'tp'), may hold values from -0.125 to 0.125
- value_projection: bfloat16 [2048, 1024], P('sp', 'tp'), may hold values from -0.125 to 0.125
- pooling_input_projection: bfloat16 [2048, 1024], P('sp', 'tp'), may hold values from -0.125 to 0.125
- decay_input_weight: bfloat16 [2048, 128], P('sp'), may hold values from -0.125 to 0.125
- rate_input_weight: bfloat16 [2048, 128], P('sp'), may hold values from -0.125 to 0.125
- gate_input_weight: bfloat16 [2048, 256], P('sp'), may hold values from -0.125 to 0.125
- decay_output_weight: bfloat16 [128, 1024], P(None, 'tp'), may hold values from -0.5 to 0.5
- rate_output_weight: bfloat16 [128, 1024], P(None, 'tp'), may hold values from -0.5 to 0.5
- gate_output_weight: bfloat16 [256, 1024], P(None, 'tp'), may hold values from -0.375 to 0.375
- decay_bias_base: float32 [1024], P('tp'), may hold values from -13 to -2.5
- learning_rate_base: float32 [1024], P('tp'), may hold values from -4 to 4
- key_prenorm_scale: float32 [1024], P('tp'), may hold values from 0.1 to 1.9
- key_learning_scale: float32 [1024], P('tp'), may hold values from 0.1 to 1.9
- self_term_weight: float32 [1024], P('tp'), may hold values from -3 to 3
- head_norm_scale: float32 [1024], P('tp'), may hold values from 0.1 to 1.9
- head_norm_bias: float32 [1024], P('tp'), may hold values from -3 to 3
- rate_extra_log: float32 [2048, 1024], P('sp', 'tp'), may hold values from -0.7 to 0.7
- decay_extra_log: float32 [2048, 1024], P('sp', 'tp'), may hold values from -0.7 to 0
- starting_head_state: float32 [16, 64, 64], P('tp'), may hold values from -12 to 12
- pooling_group_matrix: bfloat16 [8, 128, 128], P('tp'), may hold values from -0.5 to 0.5
- pooling_output_scale: float32 [1024], P('tp'), may hold values from 0.1 to 1.9
- output_attention_rows: bfloat16 [1024, 2048], P('tp', 'sp'), may hold values from -0.125 to 0.125
- output_pooling_rows: bfloat16 [1024, 2048], P('tp', 'sp'), may hold values from -0.125 to 0.125
Outputs:
- mixed: bfloat16 [2048, 2048], P(('sp', 'tp'))
The draws below stay inside these ranges and needn't reach their ends.
All inputs are finite; a program needn't handle non-finite values.
Results may differ from the reference program's by a relative error of at most 0.019.
Values may be sent and summed in bfloat16 or wider, within the bound.
A program may use at most 128 MiB of HBM per device.

```python
import jax
import jax.numpy as jnp
from jax import lax

D = 2048
HEAD_CHANNELS = 64
RWKV_HEADS = 16
POOL_GROUPS = 8
POOL_GROUP = 128
DECAY_RANK = 128
RATE_RANK = 128
GATE_RANK = 256
TOK_DEV = 128
MIXER_CHANNELS = 1024
POOL_WIDTH = 1024
SEQUENCE_LENGTH = 2048
N_TP = 2


def draw_decay_bias_base(key, part):
    first, second, third = jax.random.split(jax.random.fold_in(key, 11), 3)
    share = 0.5
    slow_heads = jax.random.uniform(first, (RWKV_HEADS,), jnp.float32) < share
    slow_mask = jnp.repeat(slow_heads, HEAD_CHANNELS)
    slow_value = jnp.log(0.5 / SEQUENCE_LENGTH) + jax.random.uniform(second, (MIXER_CHANNELS,), jnp.float32, -1.5, 0.5)
    fast_value = jax.random.uniform(third, (MIXER_CHANNELS,), jnp.float32, -3.5, -2.5)
    return jnp.where(slow_mask, slow_value, fast_value).astype(jnp.float32)


def draw_rate_extra_log(key, part):
    blocks = SEQUENCE_LENGTH // TOK_DEV
    level = jax.random.uniform(jax.random.fold_in(key, 22), (blocks, RWKV_HEADS), jnp.float32, -0.7, 0.7)
    level = jnp.repeat(level, TOK_DEV, axis=0)
    return jnp.repeat(level, HEAD_CHANNELS, axis=1).astype(jnp.float32)


def draw_decay_extra_log(key, part):
    first, second = jax.random.split(jax.random.fold_in(key, 31), 2)
    expected_output = 8.0
    rate_probability = jax.random.uniform(first, (SEQUENCE_LENGTH, RWKV_HEADS), jnp.float32)
    stack_depth = jax.random.uniform(second, (SEQUENCE_LENGTH, RWKV_HEADS), jnp.float32, 0.2, 0.5)
    decay_offset = jnp.where(rate_probability < expected_output / SEQUENCE_LENGTH, jnp.log1p(-stack_depth), 0.0)
    return jnp.repeat(decay_offset, HEAD_CHANNELS, axis=1).astype(jnp.float32)


def levels(stream_key, extent, shards, smallest, largest):
    factor_of = 1.0
    for axis_at, parts in shards:
        heights = jax.random.uniform(jax.random.fold_in(jax.random.fold_in(stream_key, 6), axis_at), (parts,), jnp.float32, smallest / len(shards), largest / len(shards))
        factor_of = factor_of * jnp.repeat(jnp.exp(heights), extent[axis_at] // parts).reshape((-1,) + (1,) * (len(extent) - 1 - axis_at))
    return factor_of


def centred(own_key, shape, scale, reach, shards=(), held_as=jnp.bfloat16):
    values = jax.random.normal(own_key, shape, jnp.float32) * scale
    if len(shards) > 0:
        values = levels(own_key, shape, shards, -0.22, 0.18) * values
    return jnp.clip(values, min=-reach, max=reach).astype(held_as)


def setup_inputs(seed: int = 0) -> dict:
    seeds = jax.random.split(jax.random.key(seed), 28)
    tokens = centred(seeds[0], (SEQUENCE_LENGTH, D), 1.0, 6.0, ((0, 16),))
    input_norm_scale = jnp.clip(1.0 + 0.18 * jax.random.normal(seeds[1], (D,), jnp.float32), 0.1, 1.9)
    input_norm_bias = centred(seeds[2], (D,), 0.3, 2.0, (), jnp.float32)
    query_projection = centred(seeds[3], (D, MIXER_CHANNELS), D ** -0.5, 0.125, ((0, 16), (1, 2)))
    key_projection = centred(seeds[4], (D, MIXER_CHANNELS), D ** -0.5, 0.125, ((0, 16), (1, 2)))
    value_projection = centred(seeds[5], (D, MIXER_CHANNELS), D ** -0.5, 0.125, ((0, 16), (1, 2)))
    pooling_input_projection = centred(seeds[6], (D, POOL_WIDTH), D ** -0.5, 0.125, ((0, 16), (1, 2)))
    decay_input_weight = centred(seeds[7], (D, DECAY_RANK), D ** -0.5, 0.125, ((0, 16),))
    rate_input_weight = centred(seeds[8], (D, RATE_RANK), D ** -0.5, 0.125, ((0, 16),))
    gate_input_weight = centred(seeds[9], (D, GATE_RANK), D ** -0.5, 0.125, ((0, 16),))
    decay_output_weight = centred(seeds[10], (DECAY_RANK, MIXER_CHANNELS), DECAY_RANK ** -0.5, 0.5, ((1, 2),))
    rate_output_weight = centred(seeds[11], (RATE_RANK, MIXER_CHANNELS), RATE_RANK ** -0.5, 0.5, ((1, 2),))
    gate_output_weight = centred(seeds[12], (GATE_RANK, MIXER_CHANNELS), GATE_RANK ** -0.5, 0.375, ((1, 2),))
    decay_bias_base = draw_decay_bias_base(jax.random.fold_in(seeds[27], 71), 0)
    learning_rate_base = centred(seeds[14], (MIXER_CHANNELS,), 1.0, 4.0, ((0, 2),), jnp.float32)
    key_prenorm_scale = jnp.clip(1.0 + 0.18 * jax.random.normal(seeds[15], (MIXER_CHANNELS,), jnp.float32), 0.1, 1.9)
    key_learning_scale = jnp.clip(1.0 + 0.18 * jax.random.normal(seeds[16], (MIXER_CHANNELS,), jnp.float32), 0.1, 1.9)
    self_term_weight = centred(seeds[17], (MIXER_CHANNELS,), 0.5, 3.0, ((0, 2),), jnp.float32)
    head_norm_scale = jnp.clip(1.0 + 0.18 * jax.random.normal(seeds[18], (MIXER_CHANNELS,), jnp.float32), 0.1, 1.9)
    head_norm_bias = centred(seeds[19], (MIXER_CHANNELS,), 0.5, 3.0, ((0, 2),), jnp.float32)
    rate_extra_log = draw_rate_extra_log(jax.random.fold_in(seeds[27], 71), 0)
    decay_extra_log = draw_decay_extra_log(jax.random.fold_in(seeds[27], 71), 0)
    starting_head_state = centred(seeds[22], (RWKV_HEADS, HEAD_CHANNELS, HEAD_CHANNELS), 2.0, 12.0, ((0, 2),), jnp.float32)
    pooling_group_matrix = centred(seeds[23], (POOL_GROUPS, POOL_GROUP, POOL_GROUP), POOL_GROUP ** -0.5, 0.5, ((0, 2),))
    pooling_output_scale = jnp.clip(1.0 + 0.18 * jax.random.normal(seeds[24], (POOL_WIDTH,), jnp.float32), 0.1, 1.9)
    output_attention_rows = centred(seeds[25], (MIXER_CHANNELS, D), D ** -0.5, 0.125, ((0, 2), (1, 16)))
    output_pooling_rows = centred(seeds[26], (POOL_WIDTH, D), D ** -0.5, 0.125, ((0, 2), (1, 16)))
    return dict(tokens=tokens, input_norm_scale=input_norm_scale, input_norm_bias=input_norm_bias, query_projection=query_projection, key_projection=key_projection, value_projection=value_projection, pooling_input_projection=pooling_input_projection, decay_input_weight=decay_input_weight, rate_input_weight=rate_input_weight, gate_input_weight=gate_input_weight, decay_output_weight=decay_output_weight, rate_output_weight=rate_output_weight, gate_output_weight=gate_output_weight, decay_bias_base=decay_bias_base, learning_rate_base=learning_rate_base, key_prenorm_scale=key_prenorm_scale, key_learning_scale=key_learning_scale, self_term_weight=self_term_weight, head_norm_scale=head_norm_scale, head_norm_bias=head_norm_bias, rate_extra_log=rate_extra_log, decay_extra_log=decay_extra_log, starting_head_state=starting_head_state, pooling_group_matrix=pooling_group_matrix, pooling_output_scale=pooling_output_scale, output_attention_rows=output_attention_rows, output_pooling_rows=output_pooling_rows)


pool_windows = (2, 4, 8, 16)
pool_reach = 16

def layer_normed(values, gain, bias):
    wide = values.astype(jnp.float32)
    center = lax.optimization_barrier(jnp.mean(wide, axis=-1, keepdims=True))
    spread = lax.optimization_barrier(jnp.mean(jnp.square(wide - center), axis=-1, keepdims=True))
    return ((wide - center) * lax.rsqrt(spread + 1e-05) * gain + bias).astype(jnp.bfloat16)

def delta_step(state, inputs):
    recv, decay_t, key_t, value_t, alpha_t, beta_t = inputs
    along = jnp.einsum('hvk,hk->hv', state, alpha_t, precision=lax.Precision.HIGHEST)
    state = state * decay_t[:, None, :] + along[:, :, None] * beta_t[:, None, :] + value_t[:, :, None] * key_t[:, None, :]
    reading = jnp.einsum('hvk,hk->hv', state, recv, precision=lax.Precision.HIGHEST)
    return (state, reading)

def window_width(scale_index):
    result = jnp.zeros(scale_index.shape, jnp.float32)
    for level, width in enumerate(pool_windows):
        result = jnp.where(scale_index == level, jnp.float32(width), result)
    return result

def window_sums(extended, scale_index, row_total):
    running = jnp.zeros((row_total, extended.shape[1]), jnp.float32)
    chosen = jnp.zeros((row_total, extended.shape[1]), jnp.float32)
    for offset in range(pool_reach):
        running = running + extended[pool_reach - offset:pool_reach - offset + row_total]
        for level, width in enumerate(pool_windows):
            if offset + 1 == width:
                chosen = jnp.where(scale_index[None, :] == level, running, chosen)
    return chosen

def reference(tokens, input_norm_scale, input_norm_bias, query_projection, key_projection, value_projection, pooling_input_projection, decay_input_weight, rate_input_weight, gate_input_weight, decay_output_weight, rate_output_weight, gate_output_weight, decay_bias_base, learning_rate_base, key_prenorm_scale, key_learning_scale, self_term_weight, head_norm_scale, head_norm_bias, rate_extra_log, decay_extra_log, starting_head_state, pooling_group_matrix, pooling_output_scale, output_attention_rows, output_pooling_rows):
    f32 = jnp.float32
    bf16 = jnp.bfloat16
    normed = layer_normed(tokens, input_norm_scale, input_norm_bias)

    def project(weight):
        return jnp.dot(normed, weight, preferred_element_type=f32).astype(bf16)
    recept, keys, values, pool_in = (project(query_projection), project(key_projection), project(value_projection), project(pooling_input_projection))
    decay_low, rate_low, gate_low = (project(decay_input_weight), project(rate_input_weight), project(gate_input_weight))
    decay_tanh = jnp.tanh(decay_low.astype(f32)).astype(bf16)
    gate_sig = jax.nn.sigmoid(gate_low.astype(f32)).astype(bf16)
    rate_logarithm = -jax.nn.softplus(-(decay_bias_base + jnp.dot(decay_tanh, decay_output_weight, preferred_element_type=f32))) - 0.5 + rate_extra_log
    decay_factor = jnp.exp(-jnp.exp(rate_logarithm) + decay_extra_log)
    rate = jax.nn.sigmoid(learning_rate_base + jnp.dot(rate_low, rate_output_weight, preferred_element_type=f32))
    gate = jnp.dot(gate_sig, gate_output_weight, preferred_element_type=f32)
    row_total = tokens.shape[0]

    def head_number(array):
        return array.astype(f32).reshape(row_total, RWKV_HEADS, HEAD_CHANNELS)

    def channel_heads(vector):
        return vector.astype(f32).reshape(RWKV_HEADS, HEAD_CHANNELS)
    key_wide = keys.astype(f32)
    unit = head_number(key_wide * key_prenorm_scale)
    unit = unit * lax.rsqrt(lax.optimization_barrier(jnp.sum(unit * unit, axis=-1, keepdims=True)) + 1e-06)
    effective_key = head_number(key_wide * (1.0 + (rate - 1.0) * key_learning_scale))
    query_per_head, value_per_head = (head_number(recept), head_number(values))
    _, reading = lax.scan(delta_step, starting_head_state.astype(f32), (query_per_head, head_number(decay_factor), effective_key, value_per_head, -unit, unit * head_number(rate)))
    center = lax.optimization_barrier(jnp.mean(reading, axis=-1, keepdims=True))
    spread = lax.optimization_barrier(jnp.mean(jnp.square(reading - center), axis=-1, keepdims=True))
    split_by_head = (reading - center) * lax.rsqrt(spread + 1e-05 * HEAD_CHANNELS) * channel_heads(head_norm_scale) + channel_heads(head_norm_bias)
    split_by_head = split_by_head + lax.optimization_barrier(jnp.sum(query_per_head * effective_key * channel_heads(self_term_weight), axis=-1, keepdims=True)) * value_per_head
    attn_out = (split_by_head.reshape(row_total, MIXER_CHANNELS) * gate).astype(bf16)
    pool_wide = pool_in.astype(f32)
    extended = jnp.concatenate([jnp.zeros((pool_reach, POOL_WIDTH), f32), pool_wide], axis=0)
    scale_index = jnp.arange(POOL_WIDTH, dtype=jnp.int32) // POOL_GROUP // (POOL_GROUPS // 4)
    chosen = window_sums(extended, scale_index, row_total)
    position = jnp.arange(row_total, dtype=jnp.int32).astype(f32)
    counted = jnp.minimum(position[:, None] + 1.0, window_width(scale_index)[None, :])
    pooled = (chosen / counted - pool_wide).astype(bf16)
    grouped = jnp.einsum('tgc,gcd->tgd', pooled.reshape(row_total, POOL_GROUPS, POOL_GROUP).astype(f32), pooling_group_matrix.astype(f32))
    pool_out = (grouped.reshape(row_total, POOL_WIDTH) * pooling_output_scale).astype(bf16)
    mix_cols = MIXER_CHANNELS // N_TP
    pool_cols = POOL_WIDTH // N_TP
    total = jnp.zeros((row_total, D), f32)
    for block in range(N_TP):
        term = jnp.dot(attn_out[:, block * mix_cols:(block + 1) * mix_cols], output_attention_rows[block * mix_cols:(block + 1) * mix_cols], preferred_element_type=f32)
        term = term + jnp.dot(pool_out[:, block * pool_cols:(block + 1) * pool_cols], output_pooling_rows[block * pool_cols:(block + 1) * pool_cols], preferred_element_type=f32)
        total = total + term.astype(bf16).astype(f32)
    return total.astype(bf16)
```

```python
import functools
import math

import jax
import jax.numpy as jnp
from jax import lax
from jax.experimental import pallas as pl
from jax.experimental.pallas import tpu as pltpu
from jax.sharding import PartitionSpec as P

HEAD_CHANNELS = 64
POOL_GROUPS = 8
POOL_GROUP = 128

pool_windows = (2, 4, 8, 16)
pool_reach = 16
span_most = 64
highest = lax.Precision.HIGHEST
f32 = jnp.float32
bf16 = jnp.bfloat16
MESH = pl.DeviceIdType.MESH
VMEM_LIMIT = 56 * 1024 * 1024

MM = (((1,), (0,)), ((), ()))
MT = (((1,), (1,)), ((), ()))
TM = (((0,), (0,)), ((), ()))


def split(a):
    high = a.astype(bf16)
    return high, (a - high.astype(f32)).astype(bf16)


def dot1(a, b, dims):
    return lax.dot_general(a, b, dims, preferred_element_type=f32)


def mm3(a, b, dims=MM):
    ah, al = split(a)
    bh, bl = split(b)
    return dot1(ah, bh, dims) + (dot1(ah, bl, dims) + dot1(al, bh, dims))


def mm2(a, b, dims=MM):
    ah, al = split(a)
    return dot1(ah, b, dims) + dot1(al, b, dims)


def passed_along(value, axis, steps):
    count = lax.axis_size(axis)
    leading, last = (max(0, -steps), min(count, count - steps))
    return lax.ppermute(value, axis, [(source, source + steps) for source in range(leading, last)])


def remote(src, dst, send, recv, peer):
    return pltpu.make_async_remote_copy(
        src_ref=src, dst_ref=dst, send_sem=send, recv_sem=recv,
        device_id={"sp": peer}, device_id_type=MESH,
    )


def project_kernel(n, group, normed_ref, w_ref, out_ref, nall, wall, res, got,
                   own_sem, ns, nr, ws, wr, rs, rr):
    me = lax.axis_index("sp")
    lo = lax.rem(me, group)
    base = me - lo
    rows = normed_ref.shape[0]
    deep = w_ref.shape[1]
    wide = w_ref.shape[2]
    barrier = pltpu.get_barrier_semaphore()
    for j in range(1, n):
        pl.semaphore_signal(barrier, inc=1, device_id={"sp": lax.rem(me + j, n)}, device_id_type=MESH)
    pl.semaphore_wait(barrier, n - 1)

    def row_slot(index, size):
        return pl.ds(pl.multiple_of(index * size, size), size)

    def w_copy(j):
        peer = lax.rem(me + j, n)
        return remote(w_ref.at[lax.rem(peer, group)], wall.at[row_slot(me, deep)],
                      ws.at[j], wr.at[j], peer)

    def w_land(j):
        source = lax.rem(me + n - j, n)
        return remote(w_ref.at[0], wall.at[row_slot(source, deep)], ws.at[j], wr.at[j], source)

    def n_copy(j):
        return remote(normed_ref, nall.at[row_slot(lo, rows)], ns.at[j], nr.at[j],
                      base + lax.rem(lo + j, group))

    def n_land(j):
        at = lax.rem(lo + group - j, group)
        return remote(normed_ref, nall.at[row_slot(at, rows)], ns.at[j], nr.at[j], base + at)

    for j in range(1, group):
        n_copy(j).start()
    for j in range(1, n):
        w_copy(j).start()
    own = (
        pltpu.make_async_copy(normed_ref, nall.at[row_slot(lo, rows)], own_sem.at[0]),
        pltpu.make_async_copy(w_ref.at[lo], wall.at[row_slot(me, deep)], own_sem.at[1]),
    )
    for c in own:
        c.start()
    for c in own:
        c.wait()
    for j in range(1, group):
        n_land(j).wait_recv()
    for j in range(1, n):
        w_land(j).wait_recv()
    weights = wall[...]
    for j in range(1, group):
        at = lax.rem(lo + j, group)
        part = jnp.dot(nall[row_slot(at, rows), :], weights, preferred_element_type=f32)
        res[j] = part.astype(bf16)
        remote(res.at[j], got.at[j], rs.at[j], rr.at[j], base + at).start()
    got[0] = jnp.dot(normed_ref[...], weights, preferred_element_type=f32).astype(bf16)
    for j in range(1, group):
        n_copy(j).wait_send()
    for j in range(1, n):
        w_copy(j).wait_send()
    for j in range(1, group):
        c = remote(res.at[j], got.at[j], rs.at[j], rr.at[j], base + lax.rem(lo + j, group))
        c.wait_send()
        c.wait_recv()
    for col in range(group):
        out_ref[:, col * wide:(col + 1) * wide] = got[lax.rem(lo + group - col, group)]


def project(normed, weights, n, group):
    rows, width = normed.shape
    _, deep, wide = weights.shape
    dma = pltpu.SemaphoreType.DMA
    return pl.pallas_call(
        functools.partial(project_kernel, n, group),
        out_shape=jax.ShapeDtypeStruct((rows, group * wide), bf16),
        in_specs=[pl.BlockSpec(memory_space=pltpu.VMEM)] * 2,
        out_specs=pl.BlockSpec(memory_space=pltpu.VMEM),
        scratch_shapes=[
            pltpu.VMEM((group * rows, width), bf16),
            pltpu.VMEM((n * deep, wide), bf16),
            pltpu.VMEM((group, rows, wide), bf16),
            pltpu.VMEM((group, rows, wide), bf16),
            dma((2,)),
            dma((group,)), dma((group,)), dma((n,)), dma((n,)), dma((group,)), dma((group,)),
        ],
        compiler_params=pltpu.CompilerParams(
            collective_id=0, has_side_effects=True, vmem_limit_bytes=VMEM_LIMIT
        ),
        cost_estimate=pl.CostEstimate(flops=10**11, bytes_accessed=10**7, transcendentals=0),
        name="project",
    )(normed, weights)


def halves(parts):
    return parts[0] if len(parts) == 1 else jnp.concatenate(parts, axis=1)


def recur_kernel(span, q_ref, k_ref, v_ref, gl_ref, dl_ref, rl_ref, gw_ref, dw_ref, rw_ref,
                 vec_ref, re_ref, de_ref, yl_ref, ym_ref, bonus_ref, gate_ref, ms_ref):
    hc = HEAD_CHANNELS
    T = q_ref.shape[0]
    heads = q_ref.shape[1] // hc
    vec = vec_ref[...]
    dbase, lbase, kscale, klearn, selfw = (vec[i:i + 1] for i in range(5))
    tanh_low = jnp.tanh(dl_ref[...].astype(f32)).astype(bf16)
    z = dbase + jnp.dot(tanh_low, dw_ref[...], preferred_element_type=f32)
    logw = de_ref[...] - jax.nn.sigmoid(z) * jnp.exp(re_ref[...] - 0.5)
    rate = jax.nn.sigmoid(lbase + jnp.dot(rl_ref[...], rw_ref[...], preferred_element_type=f32))
    sig_low = jax.nn.sigmoid(gl_ref[...].astype(f32)).astype(bf16)
    gate_ref[...] = jnp.dot(sig_low, gw_ref[...], preferred_element_type=f32)
    q = q_ref[...].astype(f32)
    k = k_ref[...].astype(f32)
    v = v_ref[...].astype(f32)
    unit = k * kscale
    keff = k * (1.0 + (rate - 1.0) * klearn)
    qkw = q * keff * selfw

    rows = lax.broadcasted_iota(jnp.int32, (T, T), 0)
    cols = lax.broadcasted_iota(jnp.int32, (T, T), 1)
    strict = rows > cols
    upto = rows >= cols
    total = jnp.dot(upto.astype(f32), logw, precision=highest, preferred_element_type=f32)
    before = total - logw
    ending = total[T - 1:T]

    def per(array):
        return [array[:, h * hc:(h + 1) * hc] for h in range(heads)]

    norms = [u * lax.rsqrt(jnp.sum(u * u, axis=1, keepdims=True) + 1e-6) for u in per(unit)]
    unit = halves(norms)
    bonus_ref[...] = halves(
        [jnp.sum(a, axis=1, keepdims=True) * b for a, b in zip(per(qkw), per(v))]
    )
    alpha = -unit
    beta = unit * rate
    center = jnp.concatenate(
        [
            jnp.broadcast_to(total[c + span // 2:c + span // 2 + 1], (span, total.shape[1]))
            for c in range(0, T, span)
        ],
        axis=0,
    )
    down = jnp.exp(center - total)
    fa = jnp.concatenate([alpha * jnp.exp(before - center), q * jnp.exp(total - center)], axis=0)
    fb = jnp.concatenate([beta * down, keff * down], axis=0)
    pair = [mm3(a, b, MT) for a, b in zip(per(fa), per(fb))]
    same = (rows // span) == (cols // span)
    lower = jnp.concatenate(
        [
            jnp.concatenate([same & strict] * 2, axis=1),
            jnp.concatenate([same & upto] * 2, axis=1),
        ],
        axis=0,
    )
    pair = [jnp.where(lower, p, 0.0) for p in pair]
    for edge in range(span, T, span):
        at = total[edge - 1:edge]
        past = jnp.exp(jnp.minimum(at - total, 0.0))
        ga = jnp.concatenate(
            [alpha * jnp.exp(jnp.minimum(before - at, 0.0)), q * jnp.exp(jnp.minimum(total - at, 0.0))],
            axis=0,
        )
        gb = jnp.concatenate([beta * past, keff * past], axis=0)
        cross = ((rows // span) == (edge // span)) & (cols < edge)
        cross = jnp.concatenate([jnp.concatenate([cross] * 2, axis=1)] * 2, axis=0)
        pair = [
            jnp.where(cross, mm3(a, b, MT), p) for a, b, p in zip(per(ga), per(gb), pair)
        ]
    la = [p[:T, :T] for p in pair]
    lb = [p[:T, T:] for p in pair]
    rb = [p[T:, :T] for p in pair]
    rk = [p[T:, T:] for p in pair]

    def joins(size):
        return ((rows // (2 * size)) == (cols // (2 * size))) & ((rows // size) != (cols // size))

    eye = (rows == cols).astype(f32)
    inverse = [eye + jnp.where(joins(1), a, 0.0) for a in la]
    size = 2
    while size < T:
        m = joins(size)
        mid = [mm3(jnp.where(m, a, 0.0), x) for a, x in zip(la, inverse)]
        inverse = [x + mm3(x, y) for x, y in zip(inverse, mid)]
        size *= 2
    ahat = per(alpha * jnp.exp(before))
    rhat = per(q * jnp.exp(total))
    values = [a.astype(bf16) for a in per(v)]
    right = [jnp.concatenate([a, mm2(b, w)], axis=1) for a, b, w in zip(ahat, lb, values)]
    wu = [mm3(x, r) for x, r in zip(inverse, right)]
    y = [mm3(b, r) for b, r in zip(rb, wu)]
    own = [mm2(b, w) for b, w in zip(rk, values)]
    ym_ref[...] = halves([r + a[:, :hc] for r, a in zip(rhat, y)])
    yl_ref[...] = halves([o + a[:, hc:] for o, a in zip(own, y)])
    tail = jnp.exp(ending - total)
    bend = per(beta * tail)
    kend = per(keff * tail)
    ie = lax.broadcasted_iota(jnp.int32, (hc, hc), 0)
    je = lax.broadcasted_iota(jnp.int32, (hc, hc), 1)
    last = per(jnp.exp(ending))
    for h in range(heads):
        both = mm3(wu[h], bend[h], TM)
        kh, kl = split(kend[h])
        added = dot1(values[h], kh, TM) + dot1(values[h], kl, TM)
        grown = jnp.where(ie == je, jnp.broadcast_to(last[h], (hc, hc)), 0.0)
        ms_ref[h] = jnp.concatenate([both[:hc] + grown, both[hc:] + added], axis=0).astype(bf16)


def recur(proj, mix, lows, gw, dw, rw, vec, re, de):
    T = proj.shape[0]
    hc = HEAD_CHANNELS
    block = math.gcd(mix, 256)
    per = block // hc
    grank, drank, rrank = lows
    heads = mix // hc
    at = 4 * mix

    def col(offset, width):
        return pl.BlockSpec((T, width), lambda i: (0, offset // width + i))

    def fixed(offset, width):
        return pl.BlockSpec((T, width), lambda i: (0, offset // width))

    def weight(rank):
        return pl.BlockSpec((rank, block), lambda i: (0, i))

    wide = jax.ShapeDtypeStruct((T, mix), f32)
    here = pl.BlockSpec((T, block), lambda i: (0, i))
    return pl.pallas_call(
        functools.partial(recur_kernel, math.gcd(span_most, T)),
        grid=(mix // block,),
        out_shape=[wide, wide, wide, wide, jax.ShapeDtypeStruct((heads, 2 * hc, hc), bf16)],
        in_specs=[
            col(0, block), col(mix, block), col(2 * mix, block),
            fixed(at, grank), fixed(at + grank, drank), fixed(at + grank + drank, rrank),
            weight(grank), weight(drank), weight(rrank),
            pl.BlockSpec((vec.shape[0], block), lambda i: (0, i)),
            here, here,
        ],
        out_specs=[here, here, here, here,
                   pl.BlockSpec((per, 2 * hc, hc), lambda i: (i, 0, 0))],
        compiler_params=pltpu.CompilerParams(vmem_limit_bytes=VMEM_LIMIT),
        cost_estimate=pl.CostEstimate(flops=6 * 10**10, bytes_accessed=10**7, transcendentals=0),
        name="recur",
    )(proj, proj, proj, proj, proj, proj, gw, dw, rw, vec, re, de)


def chain_kernel(n, group, yl_ref, ym_ref, bonus_ref, gate_ref, vec_ref, s0_ref, ms_ref, out_ref,
                 near, whole, far, ns, nr, fs, fr):
    hc = HEAD_CHANNELS
    me = lax.axis_index("sp")
    lo = lax.rem(me, group)
    base = me - lo
    hi = me // group
    groups = n // group
    heads = s0_ref.shape[0]
    near_peer = [base + lax.rem(lo + j, group) for j in range(group)]
    far_peer = [lax.rem(hi + j, groups) * group + lo for j in range(groups)]
    barrier = pltpu.get_barrier_semaphore()
    for peer in near_peer[1:] + far_peer[1:]:
        pl.semaphore_signal(barrier, inc=1, device_id={"sp": peer}, device_id_type=MESH)
    pl.semaphore_wait(barrier, group + groups - 2)
    for j in range(1, group):
        remote(ms_ref, near.at[j], ns.at[j], nr.at[j], near_peer[j]).start()
    near[0] = ms_ref[...]
    for j in range(1, group):
        remote(ms_ref, near.at[j], ns.at[j], nr.at[j], near_peer[j]).wait()
    places = [lax.rem(lo + group - l, group) for l in range(group)]
    current = [near[places[0], h].astype(f32) for h in range(heads)]
    for l in range(1, group):
        step = near[places[l]]
        current = [
            mm2(c, step[h, :hc])
            + jnp.concatenate([jnp.zeros((hc, hc), f32), step[h, hc:].astype(f32)], axis=0)
            for h, c in enumerate(current)
        ]
    for h in range(heads):
        whole[h] = current[h].astype(bf16)
    for j in range(1, groups):
        remote(whole, far.at[j], fs.at[j], fr.at[j], far_peer[j]).start()
    for j in range(1, groups):
        remote(whole, far.at[j], fs.at[j], fr.at[j], far_peer[j]).wait()
    state = [s0_ref[h] for h in range(heads)]

    def advance(state, step, go):
        return [
            jnp.where(go, mm2(s, step[h, :hc]) + step[h, hc:].astype(f32), s)
            for h, s in enumerate(state)
        ]

    for g in range(groups - 1):
        slot = jnp.maximum(lax.rem(hi + groups - g, groups), 1)
        state = advance(state, far[slot], g < hi)
    for l in range(group - 1):
        state = advance(state, near[places[l]], l < lo)
    vec = vec_ref[...]
    parts = []
    for h in range(heads):
        sl = slice(h * hc, (h + 1) * hc)
        reading = yl_ref[:, sl] + mm3(ym_ref[:, sl], state[h], MT)
        center = jnp.mean(reading, axis=1, keepdims=True)
        off = reading - center
        spread = jnp.mean(off * off, axis=1, keepdims=True)
        parts.append(off * lax.rsqrt(spread + 1e-5 * hc))
    headed = halves(parts) * vec[0:1] + vec[1:2] + bonus_ref[...]
    out_ref[...] = (headed * gate_ref[...]).astype(bf16)


def chain(yl, ym, bonus, gate, vec, s0, ms, n, group):
    heads, two, hc = ms.shape
    dma = pltpu.SemaphoreType.DMA
    groups = n // group
    return pl.pallas_call(
        functools.partial(chain_kernel, n, group),
        out_shape=jax.ShapeDtypeStruct(yl.shape, bf16),
        in_specs=[pl.BlockSpec(memory_space=pltpu.VMEM)] * 7,
        out_specs=pl.BlockSpec(memory_space=pltpu.VMEM),
        scratch_shapes=[
            pltpu.VMEM((group, heads, two, hc), bf16),
            pltpu.VMEM((heads, two, hc), bf16),
            pltpu.VMEM((groups, heads, two, hc), bf16),
            dma((group,)), dma((group,)), dma((groups,)), dma((groups,)),
        ],
        compiler_params=pltpu.CompilerParams(
            collective_id=1, has_side_effects=True, vmem_limit_bytes=VMEM_LIMIT
        ),
        cost_estimate=pl.CostEstimate(flops=4 * 10**10, bytes_accessed=10**7, transcendentals=0),
        name="chain",
    )(yl, ym, bonus, gate, vec, s0, ms)


def window_width(scale_index):
    result = jnp.zeros(scale_index.shape, jnp.float32)
    for level, width in enumerate(pool_windows):
        result = jnp.where(scale_index == level, jnp.float32(width), result)
    return result


def window_sums(extended, scale_index, row_total):
    running = jnp.zeros((row_total, extended.shape[1]), jnp.float32)
    chosen = jnp.zeros((row_total, extended.shape[1]), jnp.float32)
    for offset in range(pool_reach):
        running = running + extended[pool_reach - offset : pool_reach - offset + row_total]
        for level, width in enumerate(pool_windows):
            if offset + 1 == width:
                chosen = jnp.where(scale_index[None, :] == level, running, chosen)
    return chosen


def on_device(
    tokens,
    input_norm_scale,
    input_norm_bias,
    query_projection,
    key_projection,
    value_projection,
    pooling_input_projection,
    decay_input_weight,
    rate_input_weight,
    gate_input_weight,
    decay_output_weight,
    rate_output_weight,
    gate_output_weight,
    decay_bias_base,
    learning_rate_base,
    key_prenorm_scale,
    key_learning_scale,
    self_term_weight,
    head_norm_scale,
    head_norm_bias,
    rate_extra_log,
    decay_extra_log,
    starting_head_state,
    pooling_group_matrix,
    pooling_output_scale,
    output_attention_rows,
    output_pooling_rows,
):
    n = lax.axis_size("sp")
    group = math.gcd(n, 4)
    row_total = tokens.shape[0]
    mix_width = query_projection.shape[1]
    out_rows = lax.all_gather(
        jnp.concatenate([output_attention_rows, output_pooling_rows], axis=0), "sp", axis=0
    )
    wide = tokens.astype(f32)
    center = jnp.mean(wide, axis=-1, keepdims=True)
    spread = jnp.mean(jnp.square(wide - center), axis=-1, keepdims=True)
    normed = (
        (wide - center) * lax.rsqrt(spread + 1e-05) * input_norm_scale + input_norm_bias
    ).astype(bf16)
    weights = jnp.concatenate(
        [
            query_projection, key_projection, value_projection, pooling_input_projection,
            gate_input_weight, decay_input_weight, rate_input_weight,
        ],
        axis=1,
    )
    deep, total_cols = weights.shape
    weights = weights.reshape(deep, group, total_cols // group).transpose(1, 0, 2)
    proj = project(normed, weights, n, group)
    pool_in = proj[:, 3 * mix_width:4 * mix_width]
    lows = (gate_input_weight.shape[1], decay_input_weight.shape[1], rate_input_weight.shape[1])
    vec = jnp.stack(
        [decay_bias_base, learning_rate_base, key_prenorm_scale, key_learning_scale,
         self_term_weight, head_norm_scale, head_norm_bias, pooling_output_scale]
    )
    yl, ym, bonus, gate, ms = recur(
        proj, mix_width, lows, gate_output_weight, decay_output_weight, rate_output_weight,
        vec, rate_extra_log, decay_extra_log,
    )
    attn_out = chain(yl, ym, bonus, gate, vec[5:7], starting_head_state, ms, n, group)
    pool_width_dev = pool_in.shape[1]
    groups_dev = pool_width_dev // POOL_GROUP
    previous = passed_along(pool_in[row_total - pool_reach :], "sp", 1)
    extended = jnp.concatenate([previous, pool_in], axis=0).astype(f32)
    group_ids = (
        lax.axis_index("tp") * groups_dev
        + jnp.arange(pool_width_dev, dtype=jnp.int32) // POOL_GROUP
    )
    scale_index = group_ids // (POOL_GROUPS // 4)
    chosen = window_sums(extended, scale_index, row_total)
    position = (lax.axis_index("sp") * row_total + jnp.arange(row_total, dtype=jnp.int32)).astype(
        f32
    )
    counted = jnp.minimum(position[:, None] + 1.0, window_width(scale_index)[None, :])
    pooled = (chosen / counted - pool_in.astype(f32)).astype(bf16)
    pool_out = jnp.concatenate(
        [
            jnp.dot(pooled[:, g * POOL_GROUP:(g + 1) * POOL_GROUP], pooling_group_matrix[g],
                    preferred_element_type=f32)
            for g in range(groups_dev)
        ],
        axis=1,
    )
    pool_out = (pool_out * pooling_output_scale).astype(bf16)
    both = jnp.concatenate([attn_out, pool_out], axis=1)
    mixed = jnp.einsum("tk,skd->tsd", both, out_rows, preferred_element_type=f32)
    mixed = lax.psum_scatter(
        mixed.reshape(row_total, -1).astype(bf16), "tp", scatter_dimension=0, tiled=True
    )
    return mixed.astype(bf16)


def solution(mesh):
    in_specs = (
        P("sp", None),
        P(),
        P(),
        P("sp", "tp"),
        P("sp", "tp"),
        P("sp", "tp"),
        P("sp", "tp"),
        P("sp", None),
        P("sp", None),
        P("sp", None),
        P(None, "tp"),
        P(None, "tp"),
        P(None, "tp"),
        P("tp"),
        P("tp"),
        P("tp"),
        P("tp"),
        P("tp"),
        P("tp"),
        P("tp"),
        P("sp", "tp"),
        P("sp", "tp"),
        P("tp", None, None),
        P("tp", None, None),
        P("tp"),
        P("tp", "sp"),
        P("tp", "sp"),
    )
    out_specs = P(("sp", "tp"), None)
    return jax.shard_map(
        on_device, mesh=mesh, in_specs=in_specs, out_specs=out_specs, check_vma=False
    )
```

```python
import functools
import math

import jax
import jax.numpy as jnp
from jax import lax
from jax.experimental import pallas as pl
from jax.experimental.pallas import tpu as pltpu
from jax.sharding import PartitionSpec as P

HEAD_CHANNELS = 64
POOL_GROUPS = 8
POOL_GROUP = 128

pool_windows = (2, 4, 8, 16)
pool_reach = 16
span_most = 64
highest = lax.Precision.HIGHEST
f32 = jnp.float32
bf16 = jnp.bfloat16
MESH = pl.DeviceIdType.MESH
VMEM_LIMIT = 56 * 1024 * 1024

MM = (((1,), (0,)), ((), ()))
MT = (((1,), (1,)), ((), ()))
TM = (((0,), (0,)), ((), ()))


def split(a):
    high = a.astype(bf16)
    return high, (a - high.astype(f32)).astype(bf16)


def dot1(a, b, dims):
    return lax.dot_general(a, b, dims, preferred_element_type=f32)


def mm3(a, b, dims=MM):
    ah, al = split(a)
    bh, bl = split(b)
    return dot1(ah, bh, dims) + (dot1(ah, bl, dims) + dot1(al, bh, dims))


def mm2(a, b, dims=MM):
    ah, al = split(a)
    return dot1(ah, b, dims) + dot1(al, b, dims)


def passed_along(value, axis, steps):
    count = lax.axis_size(axis)
    leading, last = (max(0, -steps), min(count, count - steps))
    return lax.ppermute(value, axis, [(source, source + steps) for source in range(leading, last)])


def remote(src, dst, send, recv, peer):
    return pltpu.make_async_remote_copy(
        src_ref=src, dst_ref=dst, send_sem=send, recv_sem=recv,
        device_id={"sp": peer}, device_id_type=MESH,
    )


def project_kernel(n, group, pieces, tok_ref, norm_ref, *args):
    mats = args[:7]
    (oa_ref, op_ref, out_ref, ow_ref, wown, nall, wall, res, got, asm_sem, own_sem,
     ns, nr, ws, wr, us, ur, ds, dr, rs, rr, oas, oar, ops, opr) = args[7:]
    me = lax.axis_index("sp")
    lo = lax.rem(me, group)
    base = me - lo
    hi = me // group
    groups = n // group
    rows = tok_ref.shape[0]
    deep, wide = wown.shape[1:]
    mix = oa_ref.shape[0]
    near_peer = [base + lax.rem(lo + j, group) for j in range(group)]
    far_at = [lax.rem(hi + j, groups) for j in range(groups)]
    far_peer = [at * group + lo for at in far_at]

    def row_slot(index, size):
        return pl.ds(pl.multiple_of(index * size, size), size)

    assemble = []
    for i, (mat, source, quarter, target, width) in enumerate(pieces):
        c = pltpu.make_async_copy(
            mats[mat].at[:, source:source + width],
            wown.at[quarter, :, target:target + width], asm_sem.at[i],
        )
        c.start()
        assemble.append(c)
    own_out = (
        pltpu.make_async_copy(oa_ref, ow_ref.at[hi, :mix], own_sem.at[2]),
        pltpu.make_async_copy(op_ref, ow_ref.at[hi, mix:], own_sem.at[3]),
    )
    for c in own_out:
        c.start()
    barrier = pltpu.get_barrier_semaphore()
    for peer in near_peer[1:] + far_peer[1:]:
        pl.semaphore_signal(barrier, inc=1, device_id={"sp": peer}, device_id_type=MESH)
    for c in assemble:
        c.wait()
    pl.semaphore_wait(barrier, group + groups - 2)

    def w_copy(j):
        return remote(wown.at[lax.rem(lo + j, group)], wall.at[row_slot(me, deep)],
                      ws.at[j], wr.at[j], near_peer[j])

    def w_land(j):
        source = base + lax.rem(lo + group - j, group)
        return remote(wown.at[0], wall.at[row_slot(source, deep)], ws.at[j], wr.at[j], source)

    def n_copy(j):
        return remote(nall.at[row_slot(lo, rows)], nall.at[row_slot(lo, rows)], ns.at[j], nr.at[j],
                      near_peer[j])

    def n_land(j):
        at = lax.rem(lo + group - j, group)
        slot = nall.at[row_slot(at, rows)]
        return remote(slot, slot, ns.at[j], nr.at[j], base + at)

    def block(index):
        return wall.at[row_slot(index, group * deep)]

    for j in range(1, group):
        w_copy(j).start()
    own_w = pltpu.make_async_copy(wown.at[lo], wall.at[row_slot(me, deep)], own_sem.at[1])
    own_w.start()
    x = tok_ref[...].astype(f32)
    off = x - jnp.mean(x, axis=1, keepdims=True)
    spread = jnp.mean(off * off, axis=1, keepdims=True)
    nall[row_slot(lo, rows), :] = (
        off * lax.rsqrt(spread + 1e-5) * norm_ref[0:1] + norm_ref[1:2]
    ).astype(bf16)
    for j in range(1, group):
        n_copy(j).start()
    own_w.wait()
    for j in range(1, group):
        w_land(j).wait_recv()

    def up(s):
        return remote(block(hi - s), block(hi - s), us.at[s], ur.at[s], me + group)

    def up_land(s):
        return remote(block(hi - 1 - s), block(hi - 1 - s), us.at[s], ur.at[s], me - group)

    def down(s):
        return remote(block(hi + s), block(hi + s), ds.at[s], dr.at[s], me - group)

    def down_land(s):
        return remote(block(hi + 1 + s), block(hi + 1 + s), ds.at[s], dr.at[s], me + group)

    def landed(s):
        @pl.when(hi - 1 - s >= 0)
        def _():
            up_land(s).wait_recv()

        @pl.when(hi + 1 + s < groups)
        def _():
            down_land(s).wait_recv()

    def sends(s, act):
        @pl.when((hi - s >= 0) & (hi + 1 < groups))
        def _():
            act(up(s))

        @pl.when((hi + s < groups) & (hi >= 1))
        def _():
            act(down(s))

    for s in range(groups - 1):
        if s > 0:
            landed(s - 1)
        sends(s, lambda c: c.start())

    def o_copies(j):
        return (
            remote(oa_ref, ow_ref.at[hi, :mix], oas.at[j], oar.at[j], far_peer[j]),
            remote(op_ref, ow_ref.at[hi, mix:], ops.at[j], opr.at[j], far_peer[j]),
        )

    def o_lands(j):
        at = lax.rem(hi + groups - j, groups)
        return (
            remote(oa_ref, ow_ref.at[at, :mix], oas.at[j], oar.at[j], at * group + lo),
            remote(op_ref, ow_ref.at[at, mix:], ops.at[j], opr.at[j], at * group + lo),
        )

    for j in range(1, groups):
        for c in o_copies(j):
            c.start()
    for j in range(1, group):
        n_land(j).wait_recv()
    if groups > 1:
        landed(groups - 2)
    weights = wall[...]

    def r_copy(j):
        return remote(res.at[j], got.at[j], rs.at[j], rr.at[j], near_peer[j])

    for j in range(1, group):
        at = lax.rem(lo + j, group)
        part = jnp.dot(nall[row_slot(at, rows), :], weights, preferred_element_type=f32)
        res[j] = part.astype(bf16)
        r_copy(j).start()
    got[0] = jnp.dot(
        nall[row_slot(lo, rows), :], weights, preferred_element_type=f32
    ).astype(bf16)
    for j in range(1, group):
        n_copy(j).wait_send()
        w_copy(j).wait_send()
    for s in range(groups - 1):
        sends(s, lambda c: c.wait_send())
    for j in range(1, group):
        r_copy(j).wait_send()
        r_copy(j).wait_recv()
    for col in range(group):
        out_ref[:, col * wide:(col + 1) * wide] = got[lax.rem(lo + group - col, group)]
    for c in own_out:
        c.wait()
    for j in range(1, groups):
        for c in o_copies(j):
            c.wait_send()
        for c in o_lands(j):
            c.wait_recv()


def project(tokens, norm, mats, out_attn, out_pool, n, group):
    rows, width = tokens.shape
    deep = mats[0].shape[0]
    total = sum(m.shape[1] for m in mats)
    wide = total // group
    groups = n // group
    mix, cpc = out_attn.shape
    pool = out_pool.shape[0]
    pieces = []
    start = 0
    for i, m in enumerate(mats):
        done = 0
        while done < m.shape[1]:
            place = start + done
            size = min(m.shape[1] - done, wide - place % wide)
            pieces.append((i, done, place // wide, place % wide, size))
            done += size
        start += m.shape[1]
    dma = pltpu.SemaphoreType.DMA
    vm = pl.BlockSpec(memory_space=pltpu.VMEM)
    return pl.pallas_call(
        functools.partial(project_kernel, n, group, tuple(pieces)),
        out_shape=[
            jax.ShapeDtypeStruct((rows, group * wide), bf16),
            jax.ShapeDtypeStruct((groups, mix + pool, cpc), bf16),
        ],
        in_specs=[vm, vm] + [pl.BlockSpec(memory_space=pl.ANY)] * len(mats) + [vm, vm],
        out_specs=[vm, vm],
        scratch_shapes=[
            pltpu.VMEM((group, deep, wide), bf16),
            pltpu.VMEM((group * rows, width), bf16),
            pltpu.VMEM((n * deep, wide), bf16),
            pltpu.VMEM((group, rows, wide), bf16),
            pltpu.VMEM((group, rows, wide), bf16),
            dma((len(pieces),)), dma((4,)),
        ] + [dma((group,))] * 4 + [dma((groups,))] * 4 + [dma((group,))] * 2 + [dma((groups,))] * 4,
        compiler_params=pltpu.CompilerParams(
            collective_id=0, has_side_effects=True, vmem_limit_bytes=VMEM_LIMIT
        ),
        cost_estimate=pl.CostEstimate(flops=10**11, bytes_accessed=10**7, transcendentals=0),
        name="project",
    )(tokens, norm, *mats, out_attn, out_pool)


def halves(parts):
    return parts[0] if len(parts) == 1 else jnp.concatenate(parts, axis=1)


def recur_kernel(span, q_ref, k_ref, v_ref, gl_ref, dl_ref, rl_ref, gw_ref, dw_ref, rw_ref,
                 vec_ref, re_ref, de_ref, yl_ref, ym_ref, bonus_ref, gate_ref, ms_ref):
    hc = HEAD_CHANNELS
    T = q_ref.shape[0]
    heads = q_ref.shape[1] // hc
    vec = vec_ref[...]
    dbase, lbase, kscale, klearn, selfw = (vec[i:i + 1] for i in range(5))
    tanh_low = jnp.tanh(dl_ref[...].astype(f32)).astype(bf16)
    z = dbase + jnp.dot(tanh_low, dw_ref[...], preferred_element_type=f32)
    logw = de_ref[...] - jax.nn.sigmoid(z) * jnp.exp(re_ref[...] - 0.5)
    rate = jax.nn.sigmoid(lbase + jnp.dot(rl_ref[...], rw_ref[...], preferred_element_type=f32))
    sig_low = jax.nn.sigmoid(gl_ref[...].astype(f32)).astype(bf16)
    gate_ref[...] = jnp.dot(sig_low, gw_ref[...], preferred_element_type=f32)
    q = q_ref[...].astype(f32)
    k = k_ref[...].astype(f32)
    v = v_ref[...].astype(f32)
    unit = k * kscale
    keff = k * (1.0 + (rate - 1.0) * klearn)
    qkw = q * keff * selfw

    rows = lax.broadcasted_iota(jnp.int32, (T, T), 0)
    cols = lax.broadcasted_iota(jnp.int32, (T, T), 1)
    strict = rows > cols
    upto = rows >= cols
    total = jnp.dot(upto.astype(f32), logw, precision=highest, preferred_element_type=f32)
    before = total - logw
    ending = total[T - 1:T]

    def per(array):
        return [array[:, h * hc:(h + 1) * hc] for h in range(heads)]

    norms = [u * lax.rsqrt(jnp.sum(u * u, axis=1, keepdims=True) + 1e-6) for u in per(unit)]
    unit = halves(norms)
    bonus_ref[...] = halves(
        [jnp.sum(a, axis=1, keepdims=True) * b for a, b in zip(per(qkw), per(v))]
    )
    alpha = -unit
    beta = unit * rate
    center = jnp.concatenate(
        [
            jnp.broadcast_to(total[c + span // 2:c + span // 2 + 1], (span, total.shape[1]))
            for c in range(0, T, span)
        ],
        axis=0,
    )
    down = jnp.exp(center - total)
    fa = jnp.concatenate([alpha * jnp.exp(before - center), q * jnp.exp(total - center)], axis=0)
    fb = jnp.concatenate([beta * down, keff * down], axis=0)
    pair = [mm3(a, b, MT) for a, b in zip(per(fa), per(fb))]
    same = (rows // span) == (cols // span)
    lower = jnp.concatenate(
        [
            jnp.concatenate([same & strict] * 2, axis=1),
            jnp.concatenate([same & upto] * 2, axis=1),
        ],
        axis=0,
    )
    pair = [jnp.where(lower, p, 0.0) for p in pair]
    for edge in range(span, T, span):
        at = total[edge - 1:edge]
        past = jnp.exp(jnp.minimum(at - total, 0.0))
        ga = jnp.concatenate(
            [alpha * jnp.exp(jnp.minimum(before - at, 0.0)), q * jnp.exp(jnp.minimum(total - at, 0.0))],
            axis=0,
        )
        gb = jnp.concatenate([beta * past, keff * past], axis=0)
        cross = ((rows // span) == (edge // span)) & (cols < edge)
        cross = jnp.concatenate([jnp.concatenate([cross] * 2, axis=1)] * 2, axis=0)
        pair = [
            jnp.where(cross, mm3(a, b, MT), p) for a, b, p in zip(per(ga), per(gb), pair)
        ]
    la = [p[:T, :T] for p in pair]
    lb = [p[:T, T:] for p in pair]
    rb = [p[T:, :T] for p in pair]
    rk = [p[T:, T:] for p in pair]

    def joins(size):
        return ((rows // (2 * size)) == (cols // (2 * size))) & ((rows // size) != (cols // size))

    eye = (rows == cols).astype(f32)
    inverse = [eye + jnp.where(joins(1), a, 0.0) for a in la]
    size = 2
    while size < T:
        m = joins(size)
        mid = [mm3(jnp.where(m, a, 0.0), x) for a, x in zip(la, inverse)]
        inverse = [x + mm3(x, y) for x, y in zip(inverse, mid)]
        size *= 2
    ahat = per(alpha * jnp.exp(before))
    rhat = per(q * jnp.exp(total))
    values = [a.astype(bf16) for a in per(v)]
    right = [jnp.concatenate([a, mm2(b, w)], axis=1) for a, b, w in zip(ahat, lb, values)]
    wu = [mm3(x, r) for x, r in zip(inverse, right)]
    y = [mm3(b, r) for b, r in zip(rb, wu)]
    own = [mm2(b, w) for b, w in zip(rk, values)]
    ym_ref[...] = halves([r + a[:, :hc] for r, a in zip(rhat, y)])
    yl_ref[...] = halves([o + a[:, hc:] for o, a in zip(own, y)])
    tail = jnp.exp(ending - total)
    bend = per(beta * tail)
    kend = per(keff * tail)
    ie = lax.broadcasted_iota(jnp.int32, (hc, hc), 0)
    je = lax.broadcasted_iota(jnp.int32, (hc, hc), 1)
    last = per(jnp.exp(ending))
    for h in range(heads):
        both = mm3(wu[h], bend[h], TM)
        kh, kl = split(kend[h])
        added = dot1(values[h], kh, TM) + dot1(values[h], kl, TM)
        grown = jnp.where(ie == je, jnp.broadcast_to(last[h], (hc, hc)), 0.0)
        ms_ref[h] = jnp.concatenate([both[:hc] + grown, both[hc:] + added], axis=0).astype(bf16)


def recur(proj, mix, lows, gw, dw, rw, vec, re, de):
    T = proj.shape[0]
    hc = HEAD_CHANNELS
    block = math.gcd(mix, 256)
    per = block // hc
    grank, drank, rrank = lows
    heads = mix // hc
    at = 4 * mix

    def col(offset, width):
        return pl.BlockSpec((T, width), lambda i: (0, offset // width + i))

    def fixed(offset, width):
        return pl.BlockSpec((T, width), lambda i: (0, offset // width))

    def weight(rank):
        return pl.BlockSpec((rank, block), lambda i: (0, i))

    wide = jax.ShapeDtypeStruct((T, mix), f32)
    here = pl.BlockSpec((T, block), lambda i: (0, i))
    return pl.pallas_call(
        functools.partial(recur_kernel, math.gcd(span_most, T)),
        grid=(mix // block,),
        out_shape=[wide, wide, wide, wide, jax.ShapeDtypeStruct((heads, 2 * hc, hc), bf16)],
        in_specs=[
            col(0, block), col(mix, block), col(2 * mix, block),
            fixed(at, grank), fixed(at + grank, drank), fixed(at + grank + drank, rrank),
            weight(grank), weight(drank), weight(rrank),
            pl.BlockSpec((vec.shape[0], block), lambda i: (0, i)),
            here, here,
        ],
        out_specs=[here, here, here, here,
                   pl.BlockSpec((per, 2 * hc, hc), lambda i: (i, 0, 0))],
        compiler_params=pltpu.CompilerParams(vmem_limit_bytes=VMEM_LIMIT),
        cost_estimate=pl.CostEstimate(flops=6 * 10**10, bytes_accessed=10**7, transcendentals=0),
        name="recur",
    )(proj, proj, proj, proj, proj, proj, gw, dw, rw, vec, re, de)


def chain_kernel(n, group, m, yl_ref, ym_ref, bonus_ref, gate_ref, vec_ref, s0_ref, ms_ref,
                 pool_ref, ow_ref, out_ref, near, whole, far, attn, act_a, act_p, res, got,
                 ns, nr, fs, fr, as_, ar, ps, pr, rs, rr):
    hc = HEAD_CHANNELS
    me = lax.axis_index("sp")
    lo = lax.rem(me, group)
    base = me - lo
    hi = me // group
    groups = n // group
    heads = s0_ref.shape[0]
    tp = lax.axis_index("tp")
    mix = attn.shape[1]
    rt, cpc = out_ref.shape[0], ow_ref.shape[2]
    near_peer = [base + lax.rem(lo + j, group) for j in range(group)]
    far_peer = [lax.rem(hi + j, groups) * group + lo for j in range(groups)]
    barrier = pltpu.get_barrier_semaphore()
    tp_at = [lax.rem(tp + d, m) for d in range(m)]
    for j in range(group):
        for d in range(m):
            if j + d > 0:
                pl.semaphore_signal(barrier, inc=1, device_id={"sp": near_peer[j], "tp": tp_at[d]},
                                    device_id_type=MESH)
    for peer in far_peer[1:]:
        pl.semaphore_signal(barrier, inc=1, device_id={"sp": peer, "tp": tp}, device_id_type=MESH)
    pl.semaphore_wait(barrier, group * m + groups - 2)
    for j in range(1, group):
        remote(ms_ref, near.at[j], ns.at[j], nr.at[j], near_peer[j]).start()
    def p_copy(j):
        return remote(pool_ref, act_p.at[j], ps.at[j], pr.at[j], near_peer[j])

    for j in range(1, group):
        p_copy(j).start()
    act_p[0] = pool_ref[...]
    near[0] = ms_ref[...]
    for j in range(1, group):
        remote(ms_ref, near.at[j], ns.at[j], nr.at[j], near_peer[j]).wait()
    places = [lax.rem(lo + group - l, group) for l in range(group)]
    current = [near[places[0], h].astype(f32) for h in range(heads)]
    for l in range(1, group):
        step = near[places[l]]
        current = [
            mm2(c, step[h, :hc])
            + jnp.concatenate([jnp.zeros((hc, hc), f32), step[h, hc:].astype(f32)], axis=0)
            for h, c in enumerate(current)
        ]
    for h in range(heads):
        whole[h] = current[h].astype(bf16)
    for j in range(1, groups):
        remote(whole, far.at[j], fs.at[j], fr.at[j], far_peer[j]).start()
    for j in range(1, groups):
        remote(whole, far.at[j], fs.at[j], fr.at[j], far_peer[j]).wait()
    state = [s0_ref[h] for h in range(heads)]

    def advance(state, step, go):
        return [
            jnp.where(go, mm2(s, step[h, :hc]) + step[h, hc:].astype(f32), s)
            for h, s in enumerate(state)
        ]

    for g in range(groups - 1):
        slot = jnp.maximum(lax.rem(hi + groups - g, groups), 1)
        state = advance(state, far[slot], g < hi)
    for l in range(group - 1):
        state = advance(state, near[places[l]], l < lo)
    vec = vec_ref[...]
    parts = []
    for h in range(heads):
        sl = slice(h * hc, (h + 1) * hc)
        reading = yl_ref[:, sl] + mm3(ym_ref[:, sl], state[h], MT)
        center = jnp.mean(reading, axis=1, keepdims=True)
        off = reading - center
        spread = jnp.mean(off * off, axis=1, keepdims=True)
        parts.append(off * lax.rsqrt(spread + 1e-5 * hc))
    headed = halves(parts) * vec[0:1] + vec[1:2] + bonus_ref[...]
    attn[...] = (headed * gate_ref[...]).astype(bf16)

    def a_copy(j):
        return remote(attn, act_a.at[j], as_.at[j], ar.at[j], near_peer[j])

    def r_copy(j, d):
        owner = base + lax.rem(lo + group - j, group)
        return pltpu.make_async_remote_copy(
            src_ref=res.at[j, tp_at[d]], dst_ref=got.at[j, d],
            send_sem=rs.at[j * m + d], recv_sem=rr.at[j * m + d],
            device_id={"sp": owner, "tp": tp_at[d]}, device_id_type=MESH,
        )

    for j in range(1, group):
        a_copy(j).start()
    for j in range(group):
        if j > 0:
            p_copy(j).wait()
            a_copy(j).wait()
        left = attn[...] if j == 0 else act_a[j]
        pooled = act_p[j]
        for g in range(groups):
            part = (
                jnp.dot(left, ow_ref[g, :mix], preferred_element_type=f32)
                + jnp.dot(pooled, ow_ref[g, mix:], preferred_element_type=f32)
            ).astype(bf16)
            for t in range(m):
                res[j, t, g] = part[t * rt:(t + 1) * rt]
        for d in range(m):
            if j + d > 0:
                r_copy(j, d).start()
    got[0, 0] = res[0, tp]
    for j in range(group):
        for d in range(m):
            if j + d > 0:
                r_copy(j, d).wait()
    for place in range(group):
        j = lax.rem(place + group - lo, group)
        total = got[j, 0].astype(f32)
        for d in range(1, m):
            total = total + got[j, d].astype(f32)
        total = total.astype(bf16)
        for g in range(groups):
            at = (g * group + place) * cpc
            out_ref[:, at:at + cpc] = total[g]


def chain(yl, ym, bonus, gate, vec, s0, ms, pool_out, out_rows, n, group, m):
    T, mix = yl.shape
    cpc = out_rows.shape[2]
    heads, two, hc = ms.shape
    dma = pltpu.SemaphoreType.DMA
    groups = n // group
    return pl.pallas_call(
        functools.partial(chain_kernel, n, group, m),
        out_shape=jax.ShapeDtypeStruct((T // m, n * cpc), bf16),
        in_specs=[pl.BlockSpec(memory_space=pltpu.VMEM)] * 9,
        out_specs=pl.BlockSpec(memory_space=pltpu.VMEM),
        scratch_shapes=[
            pltpu.VMEM((group, heads, two, hc), bf16),
            pltpu.VMEM((heads, two, hc), bf16),
            pltpu.VMEM((groups, heads, two, hc), bf16),
            pltpu.VMEM((T, mix), bf16),
            pltpu.VMEM((group, T, mix), bf16),
            pltpu.VMEM((group,) + pool_out.shape, bf16),
            pltpu.VMEM((group, m, groups, T // m, cpc), bf16),
            pltpu.VMEM((group, m, groups, T // m, cpc), bf16),
            dma((group,)), dma((group,)), dma((groups,)), dma((groups,)),
            dma((group,)), dma((group,)), dma((group,)), dma((group,)),
            dma((group * m,)), dma((group * m,)),
        ],
        compiler_params=pltpu.CompilerParams(
            collective_id=1, has_side_effects=True, vmem_limit_bytes=VMEM_LIMIT
        ),
        cost_estimate=pl.CostEstimate(flops=4 * 10**10, bytes_accessed=10**7, transcendentals=0),
        name="chain",
    )(yl, ym, bonus, gate, vec, s0, ms, pool_out, out_rows)


def window_width(scale_index):
    result = jnp.zeros(scale_index.shape, jnp.float32)
    for level, width in enumerate(pool_windows):
        result = jnp.where(scale_index == level, jnp.float32(width), result)
    return result


def window_sums(extended, scale_index, row_total):
    running = jnp.zeros((row_total, extended.shape[1]), jnp.float32)
    chosen = jnp.zeros((row_total, extended.shape[1]), jnp.float32)
    for offset in range(pool_reach):
        running = running + extended[pool_reach - offset : pool_reach - offset + row_total]
        for level, width in enumerate(pool_windows):
            if offset + 1 == width:
                chosen = jnp.where(scale_index[None, :] == level, running, chosen)
    return chosen


def on_device(
    tokens,
    input_norm_scale,
    input_norm_bias,
    query_projection,
    key_projection,
    value_projection,
    pooling_input_projection,
    decay_input_weight,
    rate_input_weight,
    gate_input_weight,
    decay_output_weight,
    rate_output_weight,
    gate_output_weight,
    decay_bias_base,
    learning_rate_base,
    key_prenorm_scale,
    key_learning_scale,
    self_term_weight,
    head_norm_scale,
    head_norm_bias,
    rate_extra_log,
    decay_extra_log,
    starting_head_state,
    pooling_group_matrix,
    pooling_output_scale,
    output_attention_rows,
    output_pooling_rows,
):
    n = lax.axis_size("sp")
    group = math.gcd(n, 4)
    row_total = tokens.shape[0]
    mix_width = query_projection.shape[1]
    mats = (
        query_projection, key_projection, value_projection, pooling_input_projection,
        gate_input_weight, decay_input_weight, rate_input_weight,
    )
    proj, out_rows = project(
        tokens, jnp.stack([input_norm_scale, input_norm_bias]), mats,
        output_attention_rows, output_pooling_rows, n, group,
    )
    pool_in = proj[:, 3 * mix_width:4 * mix_width]
    lows = (gate_input_weight.shape[1], decay_input_weight.shape[1], rate_input_weight.shape[1])
    vec = jnp.stack(
        [decay_bias_base, learning_rate_base, key_prenorm_scale, key_learning_scale,
         self_term_weight, head_norm_scale, head_norm_bias, pooling_output_scale]
    )
    yl, ym, bonus, gate, ms = recur(
        proj, mix_width, lows, gate_output_weight, decay_output_weight, rate_output_weight,
        vec, rate_extra_log, decay_extra_log,
    )
    pool_width_dev = pool_in.shape[1]
    groups_dev = pool_width_dev // POOL_GROUP
    previous = passed_along(pool_in[row_total - pool_reach :], "sp", 1)
    extended = jnp.concatenate([previous, pool_in], axis=0).astype(f32)
    group_ids = (
        lax.axis_index("tp") * groups_dev
        + jnp.arange(pool_width_dev, dtype=jnp.int32) // POOL_GROUP
    )
    scale_index = group_ids // (POOL_GROUPS // 4)
    chosen = window_sums(extended, scale_index, row_total)
    position = (lax.axis_index("sp") * row_total + jnp.arange(row_total, dtype=jnp.int32)).astype(
        f32
    )
    counted = jnp.minimum(position[:, None] + 1.0, window_width(scale_index)[None, :])
    pooled = (chosen / counted - pool_in.astype(f32)).astype(bf16)
    pool_out = jnp.concatenate(
        [
            jnp.dot(pooled[:, g * POOL_GROUP:(g + 1) * POOL_GROUP], pooling_group_matrix[g],
                    preferred_element_type=f32)
            for g in range(groups_dev)
        ],
        axis=1,
    )
    pool_out = (pool_out * pooling_output_scale).astype(bf16)
    return chain(
        yl, ym, bonus, gate, vec[5:7], starting_head_state, ms, pool_out, out_rows,
        n, group, lax.axis_size("tp"),
    )


def solution(mesh):
    in_specs = (
        P("sp", None),
        P(),
        P(),
        P("sp", "tp"),
        P("sp", "tp"),
        P("sp", "tp"),
        P("sp", "tp"),
        P("sp", None),
        P("sp", None),
        P("sp", None),
        P(None, "tp"),
        P(None, "tp"),
        P(None, "tp"),
        P("tp"),
        P("tp"),
        P("tp"),
        P("tp"),
        P("tp"),
        P("tp"),
        P("tp"),
        P("sp", "tp"),
        P("sp", "tp"),
        P("tp", None, None),
        P("tp", None, None),
        P("tp"),
        P("tp", "sp"),
        P("tp", "sp"),
    )
    out_specs = P(("sp", "tp"), None)
    return jax.shard_map(
        on_device, mesh=mesh, in_specs=in_specs, out_specs=out_specs, check_vma=False
    )
```

```python
import functools
import math

import jax
import jax.numpy as jnp
from jax import lax
from jax.experimental import pallas as pl
from jax.experimental.pallas import tpu as pltpu
from jax.sharding import PartitionSpec as P

HEAD_CHANNELS = 64
POOL_GROUPS = 8
POOL_GROUP = 128

pool_windows = (2, 4, 8, 16)
pool_reach = 16
span_most = 64
highest = lax.Precision.HIGHEST
f32 = jnp.float32
bf16 = jnp.bfloat16
MESH = pl.DeviceIdType.MESH
VMEM_LIMIT = 56 * 1024 * 1024

MM = (((1,), (0,)), ((), ()))
MT = (((1,), (1,)), ((), ()))
TM = (((0,), (0,)), ((), ()))


def split(a):
    high = a.astype(bf16)
    return high, (a - high.astype(f32)).astype(bf16)


def dot1(a, b, dims):
    return lax.dot_general(a, b, dims, preferred_element_type=f32)


def mm3(a, b, dims=MM):
    ah, al = split(a)
    bh, bl = split(b)
    return dot1(ah, bh, dims) + (dot1(ah, bl, dims) + dot1(al, bh, dims))


def mm2(a, b, dims=MM):
    ah, al = split(a)
    return dot1(ah, b, dims) + dot1(al, b, dims)


def passed_along(value, axis, steps):
    count = lax.axis_size(axis)
    leading, last = (max(0, -steps), min(count, count - steps))
    return lax.ppermute(value, axis, [(source, source + steps) for source in range(leading, last)])


def remote(src, dst, send, recv, peer):
    return pltpu.make_async_remote_copy(
        src_ref=src, dst_ref=dst, send_sem=send, recv_sem=recv,
        device_id={"sp": peer}, device_id_type=MESH,
    )


def project_kernel(n, group, pieces, tok_ref, scale_ref, bias_ref, *args):
    mats = args[:7]
    (oa_ref, op_ref, out_ref, ow_ref, wown, nall, wall, res, got, asm_sem, own_sem,
     ns, nr, ws, wr, us, ur, ds, dr, rs, rr, oas, oar, ops, opr) = args[7:]
    me = lax.axis_index("sp")
    lo = lax.rem(me, group)
    base = me - lo
    hi = me // group
    groups = n // group
    rows = tok_ref.shape[0]
    deep, wide = wown.shape[1:]
    mix = oa_ref.shape[0]
    near_peer = [base + lax.rem(lo + j, group) for j in range(group)]
    far_at = [lax.rem(hi + j, groups) for j in range(groups)]
    far_peer = [at * group + lo for at in far_at]

    def row_slot(index, size):
        return pl.ds(pl.multiple_of(index * size, size), size)

    assemble = []
    for i, (mat, source, quarter, target, width) in enumerate(pieces):
        c = pltpu.make_async_copy(
            mats[mat].at[:, source:source + width],
            wown.at[quarter, :, target:target + width], asm_sem.at[i],
        )
        c.start()
        assemble.append(c)
    own_out = (
        pltpu.make_async_copy(oa_ref, ow_ref.at[hi, :mix], own_sem.at[2]),
        pltpu.make_async_copy(op_ref, ow_ref.at[hi, mix:], own_sem.at[3]),
    )
    for c in own_out:
        c.start()
    barrier = pltpu.get_barrier_semaphore()
    for peer in near_peer[1:] + far_peer[1:]:
        pl.semaphore_signal(barrier, inc=1, device_id={"sp": peer}, device_id_type=MESH)
    for c in assemble:
        c.wait()
    pl.semaphore_wait(barrier, group + groups - 2)

    def w_copy(j):
        return remote(wown.at[lax.rem(lo + j, group)], wall.at[row_slot(me, deep)],
                      ws.at[j], wr.at[j], near_peer[j])

    def w_land(j):
        source = base + lax.rem(lo + group - j, group)
        return remote(wown.at[0], wall.at[row_slot(source, deep)], ws.at[j], wr.at[j], source)

    def n_copy(j):
        return remote(nall.at[row_slot(lo, rows)], nall.at[row_slot(lo, rows)], ns.at[j], nr.at[j],
                      near_peer[j])

    def n_land(j):
        at = lax.rem(lo + group - j, group)
        slot = nall.at[row_slot(at, rows)]
        return remote(slot, slot, ns.at[j], nr.at[j], base + at)

    def block(index, j):
        return wall.at[row_slot(index * group + lax.rem(lo + group - j, group), deep)]

    for j in range(1, group):
        w_copy(j).start()
    own_w = pltpu.make_async_copy(wown.at[lo], wall.at[row_slot(me, deep)], own_sem.at[1])
    own_w.start()

    def relay(at, sems, s, j, peer):
        return remote(block(at, j), block(at, j), sems[0].at[s * group + j],
                      sems[1].at[s * group + j], peer)

    def landed(s, j):
        @pl.when(hi - 1 - s >= 0)
        def _():
            relay(hi - 1 - s, (us, ur), s, j, me - group).wait_recv()

        @pl.when(hi + 1 + s < groups)
        def _():
            relay(hi + 1 + s, (ds, dr), s, j, me + group).wait_recv()

    def sends(s, j, act):
        @pl.when((hi - s >= 0) & (hi + 1 < groups))
        def _():
            act(relay(hi - s, (us, ur), s, j, me + group))

        @pl.when((hi + s < groups) & (hi >= 1))
        def _():
            act(relay(hi + s, (ds, dr), s, j, me - group))

    own_w.wait()
    if groups > 1:
        sends(0, 0, lambda c: c.start())
    x = tok_ref[...].astype(f32)
    off = x - jnp.mean(x, axis=1, keepdims=True)
    spread = jnp.mean(off * off, axis=1, keepdims=True)
    nall[row_slot(lo, rows), :] = (
        off * lax.rsqrt(spread + 1e-5) * scale_ref[...] + bias_ref[...]
    ).astype(bf16)
    for j in range(1, group):
        n_copy(j).start()
    for s in range(max(groups - 1, 1)):
        for j in range(group):
            if s == 0 and j > 0:
                w_land(j).wait_recv()
            if s > 0:
                landed(s - 1, j)
            if s < groups - 1 and s + j > 0:
                sends(s, j, lambda c: c.start())

    def o_copies(j):
        return (
            remote(oa_ref, ow_ref.at[hi, :mix], oas.at[j], oar.at[j], far_peer[j]),
            remote(op_ref, ow_ref.at[hi, mix:], ops.at[j], opr.at[j], far_peer[j]),
        )

    def o_lands(j):
        at = lax.rem(hi + groups - j, groups)
        return (
            remote(oa_ref, ow_ref.at[at, :mix], oas.at[j], oar.at[j], at * group + lo),
            remote(op_ref, ow_ref.at[at, mix:], ops.at[j], opr.at[j], at * group + lo),
        )

    for j in range(1, groups):
        for c in o_copies(j):
            c.start()
    for j in range(1, group):
        n_land(j).wait_recv()
    if groups > 1:
        for j in range(group):
            landed(groups - 2, j)
    weights = wall[...]

    def r_copy(j):
        return remote(res.at[j], got.at[j], rs.at[j], rr.at[j], near_peer[j])

    for j in range(1, group):
        at = lax.rem(lo + j, group)
        part = jnp.dot(nall[row_slot(at, rows), :], weights, preferred_element_type=f32)
        res[j] = part.astype(bf16)
        r_copy(j).start()
    got[0] = jnp.dot(
        nall[row_slot(lo, rows), :], weights, preferred_element_type=f32
    ).astype(bf16)
    for j in range(1, group):
        n_copy(j).wait_send()
        w_copy(j).wait_send()
    for s in range(groups - 1):
        for j in range(group):
            sends(s, j, lambda c: c.wait_send())
    for j in range(1, group):
        r_copy(j).wait_send()
        r_copy(j).wait_recv()
    for col in range(group):
        out_ref[:, col * wide:(col + 1) * wide] = got[lax.rem(lo + group - col, group)]
    for c in own_out:
        c.wait()
    for j in range(1, groups):
        for c in o_copies(j):
            c.wait_send()
        for c in o_lands(j):
            c.wait_recv()


def project(tokens, scale, bias, mats, out_attn, out_pool, n, group):
    rows, width = tokens.shape
    deep = mats[0].shape[0]
    total = sum(m.shape[1] for m in mats)
    wide = total // group
    groups = n // group
    mix, cpc = out_attn.shape
    pool = out_pool.shape[0]
    pieces = []
    start = 0
    for i, m in enumerate(mats):
        done = 0
        while done < m.shape[1]:
            place = start + done
            size = min(m.shape[1] - done, wide - place % wide)
            pieces.append((i, done, place // wide, place % wide, size))
            done += size
        start += m.shape[1]
    dma = pltpu.SemaphoreType.DMA
    vm = pl.BlockSpec(memory_space=pltpu.VMEM)
    return pl.pallas_call(
        functools.partial(project_kernel, n, group, tuple(pieces)),
        out_shape=[
            jax.ShapeDtypeStruct((rows, group * wide), bf16),
            jax.ShapeDtypeStruct((groups, mix + pool, cpc), bf16),
        ],
        in_specs=[vm, vm, vm] + [pl.BlockSpec(memory_space=pl.ANY)] * len(mats) + [vm, vm],
        out_specs=[vm, vm],
        scratch_shapes=[
            pltpu.VMEM((group, deep, wide), bf16),
            pltpu.VMEM((group * rows, width), bf16),
            pltpu.VMEM((n * deep, wide), bf16),
            pltpu.VMEM((group, rows, wide), bf16),
            pltpu.VMEM((group, rows, wide), bf16),
            dma((len(pieces),)), dma((4,)),
        ] + [dma((group,))] * 4 + [dma((groups * group,))] * 4 + [dma((group,))] * 2 + [dma((groups,))] * 4,
        compiler_params=pltpu.CompilerParams(
            collective_id=0, has_side_effects=True, vmem_limit_bytes=VMEM_LIMIT
        ),
        cost_estimate=pl.CostEstimate(flops=10**11, bytes_accessed=10**7, transcendentals=0),
        name="project",
    )(tokens, scale[None], bias[None], *mats, out_attn, out_pool)


def halves(parts):
    return parts[0] if len(parts) == 1 else jnp.concatenate(parts, axis=1)


def recur_kernel(span, q_ref, k_ref, v_ref, gl_ref, dl_ref, rl_ref, gw_ref, dw_ref, rw_ref,
                 vec_ref, re_ref, de_ref, yl_ref, ym_ref, bonus_ref, gate_ref, ms_ref):
    hc = HEAD_CHANNELS
    T = q_ref.shape[0]
    heads = q_ref.shape[1] // hc
    vec = vec_ref[...]
    dbase, lbase, kscale, klearn, selfw = (vec[i:i + 1] for i in range(5))
    tanh_low = jnp.tanh(dl_ref[...].astype(f32)).astype(bf16)
    z = dbase + jnp.dot(tanh_low, dw_ref[...], preferred_element_type=f32)
    logw = de_ref[...] - jax.nn.sigmoid(z) * jnp.exp(re_ref[...] - 0.5)
    rate = jax.nn.sigmoid(lbase + jnp.dot(rl_ref[...], rw_ref[...], preferred_element_type=f32))
    sig_low = jax.nn.sigmoid(gl_ref[...].astype(f32)).astype(bf16)
    gate_ref[...] = jnp.dot(sig_low, gw_ref[...], preferred_element_type=f32)
    q = q_ref[...].astype(f32)
    k = k_ref[...].astype(f32)
    v = v_ref[...].astype(f32)
    unit = k * kscale
    keff = k * (1.0 + (rate - 1.0) * klearn)
    qkw = q * keff * selfw

    rows = lax.broadcasted_iota(jnp.int32, (T, T), 0)
    cols = lax.broadcasted_iota(jnp.int32, (T, T), 1)
    strict = rows > cols
    upto = rows >= cols
    total = jnp.dot(upto.astype(f32), logw, precision=highest, preferred_element_type=f32)
    before = total - logw
    ending = total[T - 1:T]

    def per(array):
        return [array[:, h * hc:(h + 1) * hc] for h in range(heads)]

    norms = [u * lax.rsqrt(jnp.sum(u * u, axis=1, keepdims=True) + 1e-6) for u in per(unit)]
    unit = halves(norms)
    bonus_ref[...] = halves(
        [jnp.sum(a, axis=1, keepdims=True) * b for a, b in zip(per(qkw), per(v))]
    )
    alpha = -unit
    beta = unit * rate
    center = jnp.concatenate(
        [
            jnp.broadcast_to(total[c + span // 2:c + span // 2 + 1], (span, total.shape[1]))
            for c in range(0, T, span)
        ],
        axis=0,
    )
    down = jnp.exp(center - total)
    fa = jnp.concatenate([alpha * jnp.exp(before - center), q * jnp.exp(total - center)], axis=0)
    fb = jnp.concatenate([beta * down, keff * down], axis=0)
    pair = [mm3(a, b, MT) for a, b in zip(per(fa), per(fb))]
    same = (rows // span) == (cols // span)
    lower = jnp.concatenate(
        [
            jnp.concatenate([same & strict] * 2, axis=1),
            jnp.concatenate([same & upto] * 2, axis=1),
        ],
        axis=0,
    )
    pair = [jnp.where(lower, p, 0.0) for p in pair]
    for edge in range(span, T, span):
        at = total[edge - 1:edge]
        past = jnp.exp(jnp.minimum(at - total, 0.0))
        ga = jnp.concatenate(
            [alpha * jnp.exp(jnp.minimum(before - at, 0.0)), q * jnp.exp(jnp.minimum(total - at, 0.0))],
            axis=0,
        )
        gb = jnp.concatenate([beta * past, keff * past], axis=0)
        cross = ((rows // span) == (edge // span)) & (cols < edge)
        cross = jnp.concatenate([jnp.concatenate([cross] * 2, axis=1)] * 2, axis=0)
        pair = [
            jnp.where(cross, mm3(a, b, MT), p) for a, b, p in zip(per(ga), per(gb), pair)
        ]
    la = [p[:T, :T] for p in pair]
    lb = [p[:T, T:] for p in pair]
    rb = [p[T:, :T] for p in pair]
    rk = [p[T:, T:] for p in pair]

    def joins(size):
        return ((rows // (2 * size)) == (cols // (2 * size))) & ((rows // size) != (cols // size))

    eye = (rows == cols).astype(f32)
    inverse = [eye + jnp.where(joins(1), a, 0.0) for a in la]
    size = 2
    while size < T:
        m = joins(size)
        mid = [mm3(jnp.where(m, a, 0.0), x) for a, x in zip(la, inverse)]
        inverse = [x + mm3(x, y) for x, y in zip(inverse, mid)]
        size *= 2
    ahat = per(alpha * jnp.exp(before))
    rhat = per(q * jnp.exp(total))
    values = [a.astype(bf16) for a in per(v)]
    right = [jnp.concatenate([a, mm2(b, w)], axis=1) for a, b, w in zip(ahat, lb, values)]
    wu = [mm3(x, r) for x, r in zip(inverse, right)]
    y = [mm3(b, r) for b, r in zip(rb, wu)]
    own = [mm2(b, w) for b, w in zip(rk, values)]
    ym_ref[...] = halves([r + a[:, :hc] for r, a in zip(rhat, y)])
    yl_ref[...] = halves([o + a[:, hc:] for o, a in zip(own, y)])
    tail = jnp.exp(ending - total)
    bend = per(beta * tail)
    kend = per(keff * tail)
    ie = lax.broadcasted_iota(jnp.int32, (hc, hc), 0)
    je = lax.broadcasted_iota(jnp.int32, (hc, hc), 1)
    last = per(jnp.exp(ending))
    for h in range(heads):
        both = mm3(wu[h], bend[h], TM)
        kh, kl = split(kend[h])
        added = dot1(values[h], kh, TM) + dot1(values[h], kl, TM)
        grown = jnp.where(ie == je, jnp.broadcast_to(last[h], (hc, hc)), 0.0)
        ms_ref[h] = jnp.concatenate([both[:hc] + grown, both[hc:] + added], axis=0).astype(bf16)


def recur(proj, mix, lows, gw, dw, rw, vec, re, de):
    T = proj.shape[0]
    hc = HEAD_CHANNELS
    block = math.gcd(mix, 256)
    per = block // hc
    grank, drank, rrank = lows
    heads = mix // hc
    at = 4 * mix

    def col(offset, width):
        return pl.BlockSpec((T, width), lambda i: (0, offset // width + i))

    def fixed(offset, width):
        return pl.BlockSpec((T, width), lambda i: (0, offset // width))

    def weight(rank):
        return pl.BlockSpec((rank, block), lambda i: (0, i))

    wide = jax.ShapeDtypeStruct((T, mix), f32)
    here = pl.BlockSpec((T, block), lambda i: (0, i))
    return pl.pallas_call(
        functools.partial(recur_kernel, math.gcd(span_most, T)),
        grid=(mix // block,),
        out_shape=[wide, wide, wide, wide, jax.ShapeDtypeStruct((heads, 2 * hc, hc), bf16)],
        in_specs=[
            col(0, block), col(mix, block), col(2 * mix, block),
            fixed(at, grank), fixed(at + grank, drank), fixed(at + grank + drank, rrank),
            weight(grank), weight(drank), weight(rrank),
            pl.BlockSpec((vec.shape[0], block), lambda i: (0, i)),
            here, here,
        ],
        out_specs=[here, here, here, here,
                   pl.BlockSpec((per, 2 * hc, hc), lambda i: (i, 0, 0))],
        compiler_params=pltpu.CompilerParams(vmem_limit_bytes=VMEM_LIMIT),
        cost_estimate=pl.CostEstimate(flops=6 * 10**10, bytes_accessed=10**7, transcendentals=0),
        name="recur",
    )(proj, proj, proj, proj, proj, proj, gw, dw, rw, vec, re, de)


def chain_kernel(n, group, m, yl_ref, ym_ref, bonus_ref, gate_ref, vec_ref, s0_ref, ms_ref,
                 pool_ref, ow_ref, out_ref, near, whole, far, attn, act_a, act_p, res, got,
                 ns, nr, fs, fr, as_, ar, ps, pr, rs, rr):
    hc = HEAD_CHANNELS
    me = lax.axis_index("sp")
    lo = lax.rem(me, group)
    base = me - lo
    hi = me // group
    groups = n // group
    heads = s0_ref.shape[0]
    tp = lax.axis_index("tp")
    mix = attn.shape[1]
    rt, cpc = out_ref.shape[0], ow_ref.shape[2]
    near_peer = [base + lax.rem(lo + j, group) for j in range(group)]
    far_peer = [lax.rem(hi + j, groups) * group + lo for j in range(groups)]
    barrier = pltpu.get_barrier_semaphore()
    tp_at = [lax.rem(tp + d, m) for d in range(m)]
    for j in range(group):
        for d in range(m):
            if j + d > 0:
                pl.semaphore_signal(barrier, inc=1, device_id={"sp": near_peer[j], "tp": tp_at[d]},
                                    device_id_type=MESH)
    for peer in far_peer[1:]:
        pl.semaphore_signal(barrier, inc=1, device_id={"sp": peer, "tp": tp}, device_id_type=MESH)
    pl.semaphore_wait(barrier, group * m + groups - 2)
    for j in range(1, group):
        remote(ms_ref, near.at[j], ns.at[j], nr.at[j], near_peer[j]).start()
    def p_copy(j):
        return remote(pool_ref, act_p.at[j], ps.at[j], pr.at[j], near_peer[j])

    for j in range(1, group):
        p_copy(j).start()
    act_p[0] = pool_ref[...]
    near[0] = ms_ref[...]
    for j in range(1, group):
        remote(ms_ref, near.at[j], ns.at[j], nr.at[j], near_peer[j]).wait()
    places = [lax.rem(lo + group - l, group) for l in range(group)]
    current = [near[places[0], h].astype(f32) for h in range(heads)]
    for l in range(1, group):
        step = near[places[l]]
        current = [
            mm2(c, step[h, :hc])
            + jnp.concatenate([jnp.zeros((hc, hc), f32), step[h, hc:].astype(f32)], axis=0)
            for h, c in enumerate(current)
        ]
    for h in range(heads):
        whole[h] = current[h].astype(bf16)
    for j in range(1, groups):
        remote(whole, far.at[j], fs.at[j], fr.at[j], far_peer[j]).start()
    for j in range(1, groups):
        remote(whole, far.at[j], fs.at[j], fr.at[j], far_peer[j]).wait()
    state = [s0_ref[h] for h in range(heads)]

    def advance(state, step, go):
        return [
            jnp.where(go, mm2(s, step[h, :hc]) + step[h, hc:].astype(f32), s)
            for h, s in enumerate(state)
        ]

    for g in range(groups - 1):
        slot = jnp.maximum(lax.rem(hi + groups - g, groups), 1)
        state = advance(state, far[slot], g < hi)
    for l in range(group - 1):
        state = advance(state, near[places[l]], l < lo)
    vec = vec_ref[...]
    parts = []
    for h in range(heads):
        sl = slice(h * hc, (h + 1) * hc)
        reading = yl_ref[:, sl] + mm3(ym_ref[:, sl], state[h], MT)
        center = jnp.mean(reading, axis=1, keepdims=True)
        off = reading - center
        spread = jnp.mean(off * off, axis=1, keepdims=True)
        parts.append(off * lax.rsqrt(spread + 1e-5 * hc))
    headed = halves(parts) * vec[0:1] + vec[1:2] + bonus_ref[...]
    attn[...] = (headed * gate_ref[...]).astype(bf16)

    def a_copy(j):
        return remote(attn, act_a.at[j], as_.at[j], ar.at[j], near_peer[j])

    def r_copy(j, d):
        owner = base + lax.rem(lo + group - j, group)
        return pltpu.make_async_remote_copy(
            src_ref=res.at[j, tp_at[d]], dst_ref=got.at[j, d],
            send_sem=rs.at[j * m + d], recv_sem=rr.at[j * m + d],
            device_id={"sp": owner, "tp": tp_at[d]}, device_id_type=MESH,
        )

    for j in range(1, group):
        a_copy(j).start()
    for j in range(group):
        if j > 0:
            p_copy(j).wait()
            a_copy(j).wait()
        left = attn[...] if j == 0 else act_a[j]
        pooled = act_p[j]
        for g in range(groups):
            part = (
                jnp.dot(left, ow_ref[g, :mix], preferred_element_type=f32)
                + jnp.dot(pooled, ow_ref[g, mix:], preferred_element_type=f32)
            ).astype(bf16)
            for t in range(m):
                res[j, t, g] = part[t * rt:(t + 1) * rt]
        for d in range(m):
            if j + d > 0:
                r_copy(j, d).start()
    got[0, 0] = res[0, tp]
    for j in range(group):
        for d in range(m):
            if j + d > 0:
                r_copy(j, d).wait()
    for place in range(group):
        j = lax.rem(place + group - lo, group)
        total = got[j, 0].astype(f32)
        for d in range(1, m):
            total = total + got[j, d].astype(f32)
        total = total.astype(bf16)
        for g in range(groups):
            at = (g * group + place) * cpc
            out_ref[:, at:at + cpc] = total[g]


def chain(yl, ym, bonus, gate, vec, s0, ms, pool_out, out_rows, n, group, m):
    T, mix = yl.shape
    cpc = out_rows.shape[2]
    heads, two, hc = ms.shape
    dma = pltpu.SemaphoreType.DMA
    groups = n // group
    return pl.pallas_call(
        functools.partial(chain_kernel, n, group, m),
        out_shape=jax.ShapeDtypeStruct((T // m, n * cpc), bf16),
        in_specs=[pl.BlockSpec(memory_space=pltpu.VMEM)] * 9,
        out_specs=pl.BlockSpec(memory_space=pltpu.VMEM),
        scratch_shapes=[
            pltpu.VMEM((group, heads, two, hc), bf16),
            pltpu.VMEM((heads, two, hc), bf16),
            pltpu.VMEM((groups, heads, two, hc), bf16),
            pltpu.VMEM((T, mix), bf16),
            pltpu.VMEM((group, T, mix), bf16),
            pltpu.VMEM((group,) + pool_out.shape, bf16),
            pltpu.VMEM((group, m, groups, T // m, cpc), bf16),
            pltpu.VMEM((group, m, groups, T // m, cpc), bf16),
            dma((group,)), dma((group,)), dma((groups,)), dma((groups,)),
            dma((group,)), dma((group,)), dma((group,)), dma((group,)),
            dma((group * m,)), dma((group * m,)),
        ],
        compiler_params=pltpu.CompilerParams(
            collective_id=1, has_side_effects=True, vmem_limit_bytes=VMEM_LIMIT
        ),
        cost_estimate=pl.CostEstimate(flops=4 * 10**10, bytes_accessed=10**7, transcendentals=0),
        name="chain",
    )(yl, ym, bonus, gate, vec, s0, ms, pool_out, out_rows)


def window_width(scale_index):
    result = jnp.zeros(scale_index.shape, jnp.float32)
    for level, width in enumerate(pool_windows):
        result = jnp.where(scale_index == level, jnp.float32(width), result)
    return result


def window_sums(extended, scale_index, row_total):
    running = jnp.zeros((row_total, extended.shape[1]), jnp.float32)
    chosen = jnp.zeros((row_total, extended.shape[1]), jnp.float32)
    for offset in range(pool_reach):
        running = running + extended[pool_reach - offset : pool_reach - offset + row_total]
        for level, width in enumerate(pool_windows):
            if offset + 1 == width:
                chosen = jnp.where(scale_index[None, :] == level, running, chosen)
    return chosen


def on_device(
    tokens,
    input_norm_scale,
    input_norm_bias,
    query_projection,
    key_projection,
    value_projection,
    pooling_input_projection,
    decay_input_weight,
    rate_input_weight,
    gate_input_weight,
    decay_output_weight,
    rate_output_weight,
    gate_output_weight,
    decay_bias_base,
    learning_rate_base,
    key_prenorm_scale,
    key_learning_scale,
    self_term_weight,
    head_norm_scale,
    head_norm_bias,
    rate_extra_log,
    decay_extra_log,
    starting_head_state,
    pooling_group_matrix,
    pooling_output_scale,
    output_attention_rows,
    output_pooling_rows,
):
    n = lax.axis_size("sp")
    group = math.gcd(n, 4)
    row_total = tokens.shape[0]
    mix_width = query_projection.shape[1]
    mats = (
        query_projection, key_projection, value_projection, pooling_input_projection,
        gate_input_weight, decay_input_weight, rate_input_weight,
    )
    proj, out_rows = project(
        tokens, input_norm_scale, input_norm_bias, mats,
        output_attention_rows, output_pooling_rows, n, group,
    )
    pool_in = proj[:, 3 * mix_width:4 * mix_width]
    lows = (gate_input_weight.shape[1], decay_input_weight.shape[1], rate_input_weight.shape[1])
    vec = jnp.stack(
        [decay_bias_base, learning_rate_base, key_prenorm_scale, key_learning_scale,
         self_term_weight, head_norm_scale, head_norm_bias, pooling_output_scale]
    )
    yl, ym, bonus, gate, ms = recur(
        proj, mix_width, lows, gate_output_weight, decay_output_weight, rate_output_weight,
        vec, rate_extra_log, decay_extra_log,
    )
    pool_width_dev = pool_in.shape[1]
    groups_dev = pool_width_dev // POOL_GROUP
    previous = passed_along(pool_in[row_total - pool_reach :], "sp", 1)
    extended = jnp.concatenate([previous, pool_in], axis=0).astype(f32)
    group_ids = (
        lax.axis_index("tp") * groups_dev
        + jnp.arange(pool_width_dev, dtype=jnp.int32) // POOL_GROUP
    )
    scale_index = group_ids // (POOL_GROUPS // 4)
    chosen = window_sums(extended, scale_index, row_total)
    position = (lax.axis_index("sp") * row_total + jnp.arange(row_total, dtype=jnp.int32)).astype(
        f32
    )
    counted = jnp.minimum(position[:, None] + 1.0, window_width(scale_index)[None, :])
    pooled = (chosen / counted - pool_in.astype(f32)).astype(bf16)
    pool_out = jnp.concatenate(
        [
            jnp.dot(pooled[:, g * POOL_GROUP:(g + 1) * POOL_GROUP], pooling_group_matrix[g],
                    preferred_element_type=f32)
            for g in range(groups_dev)
        ],
        axis=1,
    )
    pool_out = (pool_out * pooling_output_scale).astype(bf16)
    return chain(
        yl, ym, bonus, gate, vec[5:7], starting_head_state, ms, pool_out, out_rows,
        n, group, lax.axis_size("tp"),
    )


def solution(mesh):
    in_specs = (
        P("sp", None),
        P(),
        P(),
        P("sp", "tp"),
        P("sp", "tp"),
        P("sp", "tp"),
        P("sp", "tp"),
        P("sp", None),
        P("sp", None),
        P("sp", None),
        P(None, "tp"),
        P(None, "tp"),
        P(None, "tp"),
        P("tp"),
        P("tp"),
        P("tp"),
        P("tp"),
        P("tp"),
        P("tp"),
        P("tp"),
        P("sp", "tp"),
        P("sp", "tp"),
        P("tp", None, None),
        P("tp", None, None),
        P("tp"),
        P("tp", "sp"),
        P("tp", "sp"),
    )
    out_specs = P(("sp", "tp"), None)
    return jax.shard_map(
        on_device, mesh=mesh, in_specs=in_specs, out_specs=out_specs, check_vma=False
    )
```
